32 devices in a mesh: gr: 2 (over core), fs: 8 (over z, y), tp: 2 (over x).
Axes of the slice: x: 2, y: 2, z: 4, core: 2. Of those that a mesh axis runs over, the one named last changes fastest.
Arguments:
- tokens: bfloat16 [6144, 2048], P(('gr', 'fs')), may hold values from -6 to 6
- route_ids: int32 [6144, 2], P(('gr', 'fs')), may hold values from 0 to 7, as said below
- route_weights: float32 [6144, 2], P(('gr', 'fs')), may hold values from 0.1 to 1
- norm_gain: float32 [2048], P(('gr', 'fs')), may hold values from 0.1 to 1.9
- gate_weight: float32 [8, 2048, 1024], P(None, ('gr', 'fs'), 'tp'), may hold values from -0.125 to 0.125
- up_weight: float32 [8, 2048, 1024], P(None, ('gr', 'fs'), 'tp'), may hold values from -0.125 to 0.125
- down_weight: float32 [8, 1024, 2048], P(None, ('gr', 'fs'), 'tp'), may hold values from -0.1875 to 0.1875
Outputs:
- gate_new: bfloat16 [8, 2048, 1024], P('fs', None, 'tp')
- up_new: bfloat16 [8, 2048, 1024], P('fs', None, 'tp')
- down_new: bfloat16 [8, 1024, 2048], P('fs', 'tp')
- mixed: bfloat16 [6144, 2048], P(('gr', 'fs'), 'tp')
The draws below stay inside these ranges and needn't reach their ends.
Inputs may be any that keep to these rules, and one draw needn't show every extreme that they name: `route_ids`: each row names two different experts of one group (expert e belongs to group e // 2); in each device's block of 384 rows every expert is named by exactly 96 rows.
All inputs are finite; a program needn't handle non-finite values.
Results may differ from the reference program's by a relative error of at most 0.015.
Values may be sent and summed in bfloat16 or wider, within the bound.
A program may use at most 64 MiB of HBM per device.

```python
import jax
import jax.numpy as jnp
from jax import lax

D = 2048
FF = 1024
GROUPS = 4
TOK_DEV = 384
EXPERTS = 8
EPG = 2
HID_DEV = 512
TOKENS = 6144
N_GR = 2
N_FS = 8


def draw_route_ids(key, part):
    blocks = N_GR * N_FS

    def one_block(block_key):
        key_order, key_first, key_step = jax.random.split(block_key, 3)
        place = jax.random.permutation(key_order, TOK_DEV).astype(jnp.int32)
        group = place % GROUPS
        inner = place // GROUPS
        first_shift = jax.random.randint(key_first, (GROUPS,), 0, EPG).astype(jnp.int32)
        step_shift = jax.random.randint(key_step, (GROUPS,), 0, EPG - 1).astype(jnp.int32)
        first = (inner + first_shift[group]) % EPG
        stride = 1 + (inner // EPG + step_shift[group]) % (EPG - 1)
        second = (first + stride) % EPG
        return jnp.stack([group * EPG + first, group * EPG + second], axis=1).astype(jnp.int32)
    keys = jax.random.split(key, blocks)
    return jax.vmap(one_block)(keys).reshape(TOKENS, 2)


def shard_levels(stream_key, shape, cuts, low, top_value):
    gain, own = 1.0, jax.random.fold_in(stream_key, 6)
    for position, shards_of in cuts:
        draws = jnp.exp(jax.random.uniform(jax.random.fold_in(own, position), (shards_of,), jnp.float32, low / len(cuts), top_value / len(cuts)))
        gain = gain * jnp.repeat(draws, shape[position] // shards_of).reshape([-1 if axis == position else 1 for axis in range(len(shape))])
    return gain


def gaussian(own_key, shape, width, limit, cuts=(), held_as=jnp.bfloat16):
    level = shard_levels(own_key, shape, cuts, -0.22, 0.18) if cuts else 1.0
    array = jax.random.normal(own_key, shape, jnp.float32) * width * level
    return jnp.minimum(jnp.maximum(array, -limit), limit).astype(held_as)


def setup_inputs(seed: int = 0) -> dict:
    arg_keys = jax.random.split(jax.random.key(seed), 8)
    return {
        "tokens": gaussian(arg_keys[0], (TOKENS, D), 1.0, 6.0, ((0, 16),)),
        "route_ids": draw_route_ids(jax.random.fold_in(arg_keys[7], 71), 0),
        "route_weights": jnp.clip(0.1 + 0.9 * jax.random.uniform(arg_keys[2], (TOKENS, 2), jnp.float32) ** shard_levels(arg_keys[2], (TOKENS, 2), ((0, 16),), -0.2, 0.2), 0.1, 1.0),
        "norm_gain": jnp.clip(1.0 + 0.18 * jax.random.normal(arg_keys[3], (D,), jnp.float32), 0.1, 1.9),
        "gate_weight": gaussian(arg_keys[4], (EXPERTS, D, FF), D ** -0.5, 0.125, ((1, 16), (2, 2)), jnp.float32),
        "up_weight": gaussian(arg_keys[5], (EXPERTS, D, FF), D ** -0.5, 0.125, ((1, 16), (2, 2)), jnp.float32),
        "down_weight": gaussian(arg_keys[6], (EXPERTS, FF, D), FF ** -0.5, 0.1875, ((1, 16), (2, 2)), jnp.float32),
    }


def expert_block(args):
    gate_one, up_one, down_one, rows = args
    first = jnp.dot(rows, gate_one, preferred_element_type=jnp.float32)
    second = jnp.dot(rows, up_one, preferred_element_type=jnp.float32)
    hidden = (jax.nn.silu(first) * second).astype(jnp.bfloat16)
    count = rows.shape[0]
    pieces = hidden.reshape(count, FF // HID_DEV, HID_DEV).astype(jnp.float32)
    down_pieces = down_one.reshape(FF // HID_DEV, HID_DEV, D).astype(jnp.float32)
    partials = jnp.einsum('mbf,bfd->bmd', pieces, down_pieces).astype(jnp.bfloat16)
    return lax.optimization_barrier(jnp.sum(partials.astype(jnp.float32), axis=0)).astype(jnp.bfloat16)

def reference(tokens, route_ids, route_weights, norm_gain, gate_weight, up_weight, down_weight):
    gate_new = (gate_weight * norm_gain[None, :, None]).astype(jnp.bfloat16)
    up_new = (up_weight * norm_gain[None, :, None]).astype(jnp.bfloat16)
    down_new = down_weight.astype(jnp.bfloat16)
    widened = tokens.astype(jnp.float32)
    normed = (widened * lax.rsqrt(lax.optimization_barrier(jnp.mean(widened * widened, axis=-1, keepdims=True)) + 1e-06)).astype(jnp.bfloat16)
    flat_ids = route_ids.reshape(-1)
    per_expert = flat_ids.shape[0] // EXPERTS
    order = jnp.argsort(flat_ids, stable=True).astype(jnp.int32).reshape(EXPERTS, per_expert)

    def one_expert(args):
        gate_one, up_one, down_one, picks = args
        rows = normed[picks // 2]
        return expert_block((gate_one, up_one, down_one, rows))
    results = lax.map(one_expert, (gate_new, up_new, down_new, order))
    route_out = jnp.zeros((flat_ids.shape[0], D), jnp.bfloat16).at[order.reshape(-1)].set(results.reshape(-1, D))
    route_out = route_out.reshape(-1, 2, D).astype(jnp.float32)
    mixed = lax.optimization_barrier(jnp.sum(route_weights[:, :, None] * route_out, axis=1)).astype(jnp.bfloat16)
    return (gate_new, up_new, down_new, mixed)
```

```python
import functools

import jax
import jax.numpy as jnp
from jax import lax
from jax.experimental import pallas as pl
from jax.experimental.pallas import tpu as pltpu
from jax.sharding import PartitionSpec as P

GROUPS = 4
BF16 = jnp.bfloat16
MESH = pl.DeviceIdType.MESH


def local(tokens, route_ids, route_weights, norm_gain, gate_weight, up_weight, down_weight):
    gate_folded = (gate_weight * norm_gain[None, :, None]).astype(jnp.bfloat16)
    up_folded = (up_weight * norm_gain[None, :, None]).astype(jnp.bfloat16)
    down_rounded = down_weight.astype(jnp.bfloat16)
    moved = (
        lax.all_to_all(gate_folded, "fs", split_axis=0, concat_axis=1, tiled=True),
        lax.all_to_all(up_folded, "fs", split_axis=0, concat_axis=1, tiled=True),
        lax.all_to_all(down_rounded, "fs", split_axis=0, concat_axis=1, tiled=True),
    )
    gate_new, up_new, down_whole = (
        lax.all_gather(moved[0], "gr", axis=1, tiled=True),
        lax.all_gather(moved[1], "gr", axis=1, tiled=True),
        lax.all_gather(moved[2], "gr", axis=1, tiled=True),
    )
    down_new = lax.all_to_all(down_whole, "tp", split_axis=1, concat_axis=2, tiled=True)
    tok = tokens.shape[0]
    width = tokens.shape[1]
    experts = gate_weight.shape[0]
    cap = 2 * tok // experts
    flat_ids = route_ids.reshape(-1)
    onehot = (flat_ids[:, None] == jnp.arange(experts, dtype=jnp.int32)[None, :]).astype(jnp.int32)
    slot = jnp.sum(jnp.cumsum(onehot, axis=0) * onehot, axis=1) - 1
    position = flat_ids * cap + slot
    source = (
        jnp.zeros((experts * cap,), jnp.int32)
        .at[position]
        .set(jnp.arange(2 * tok, dtype=jnp.int32) // 2)
    )
    widened = tokens.astype(jnp.float32)
    normed = (
        widened * lax.rsqrt(jnp.mean(widened * widened, axis=-1, keepdims=True) + 1e-06)
    ).astype(jnp.bfloat16)
    outgoing = normed[source].reshape(experts, cap, width)
    received = lax.all_to_all(outgoing, "fs", split_axis=0, concat_axis=0, tiled=True)
    senders, count, _ = received.shape
    rows = received.reshape(senders * count, width)
    first = jnp.dot(rows, gate_new[0], preferred_element_type=jnp.float32)
    second = jnp.dot(rows, up_new[0], preferred_element_type=jnp.float32)
    hidden = (jax.nn.silu(first) * second).astype(jnp.bfloat16)
    partial_out = jnp.dot(hidden, down_new[0], preferred_element_type=jnp.float32)
    summed = lax.psum_scatter(
        partial_out.reshape(senders, count, width).astype(jnp.bfloat16),
        "tp",
        scatter_dimension=2,
        tiled=True,
    )
    returned = lax.all_to_all(summed, "fs", split_axis=0, concat_axis=0, tiled=True)
    columns = returned.shape[2]
    route_out = returned.reshape(experts * cap, columns)[position].reshape(tok, 2, columns)
    mixed = jnp.sum(route_weights[:, :, None] * route_out.astype(jnp.float32), axis=1).astype(
        jnp.bfloat16
    )
    return (gate_new, up_new, down_new, mixed)


def place(n_z, n_y):
    f = lax.axis_index("fs")
    return lax.axis_index("gr"), f // n_y, lax.rem(f, n_y), lax.axis_index("tp")


def flip(z, k):
    return (z, z + 1 - 2 * lax.rem(z, 2), lax.rem(z + 2, 4), 3 - z)[k]


def device(c, z, y, x, n_y):
    return {"gr": c, "fs": z * n_y + y, "tp": x}


def greet(peers):
    barrier = pltpu.get_barrier_semaphore()
    for peer in peers:
        pl.semaphore_signal(barrier, inc=1, device_id=peer, device_id_type=MESH)
    pl.semaphore_wait(barrier, len(peers))


def remote(src, dst, send, recv, peer):
    return pltpu.make_async_remote_copy(
        src_ref=src, dst_ref=dst, send_sem=send, recv_sem=recv,
        device_id=peer, device_id_type=MESH,
    )


def hand_over(
    n_z, n_y,
    gate_in, up_in, down_in, tok_in, rw_in,
    gate_out, up_out, down_out, rows_out, rw_out,
    w_send, w_recv, f_send, f_recv,
    tz_send, tz_recv, ty_send, ty_recv, tx_send, tx_recv,
    rz_send, rz_recv, ry_send, ry_recv, own, spare,
):
    c, z, y, x = place(n_z, n_y)
    me = z * n_y + y
    n_fs = n_z * n_y
    g_rows, d_rows = gate_in.shape[1], down_in.shape[1]
    half = tok_in.shape[2]
    dev = functools.partial(device, n_y=n_y)
    ks = [(kz, ky) for kz in (3, 2, 1, 0) for ky in (1, 0)]

    def peer_of(k):
        return flip(z, k[0]), (1 - y if k[1] else y)

    other = dev(1 - c, z, y, x)
    x_nbr = dev(c, z, y, 1 - x)
    y_nbr = dev(c, z, 1 - y, x)
    peers = [dev(c, *peer_of(k), x) for k in ks if k != (0, 0)]
    peers += [dev(x, *peer_of(k), c) for k in ks if k != (0, 0)]
    peers += [other, x_nbr, dev(1 - c, z, y, 1 - x)]
    greet(peers)

    def xcols(i):
        return pl.ds(pl.multiple_of(i * half, half), half)

    def grow(core, src):
        return pl.ds(pl.multiple_of((core * n_fs + src) * g_rows, g_rows), g_rows)

    def drow(src):
        return pl.ds(pl.multiple_of(src * d_rows, d_rows), d_rows)

    waits = []
    tz = {}
    rz = {}
    for kz in (3, 2, 1):
        g = flip(z, kz)
        peer = dev(c, g, y, x)
        tz[kz] = remote(tok_in.at[g], rows_out.at[me, :, xcols(x)],
                        tz_send.at[kz], tz_recv.at[kz], peer)
        tz[kz].start()
        rz[kz] = remote(rw_in.at[g], rw_out.at[me], rz_send.at[kz], rz_recv.at[kz], peer)
        rz[kz].start()
    own_tok = pltpu.make_async_copy(tok_in.at[z], rows_out.at[me, :, xcols(x)], own.at[0])
    own_tok.start()
    own_rw = pltpu.make_async_copy(rw_in.at[z], rw_out.at[me], own.at[1])
    own_rw.start()
    ty = {}
    tx = {}
    ry = {}
    ty[0] = remote(tok_in.at[z], rows_out.at[me, :, xcols(x)], ty_send.at[0], ty_recv.at[0], y_nbr)
    ty[0].start()
    ry[0] = remote(rw_in.at[z], rw_out.at[me], ry_send.at[0], ry_recv.at[0], y_nbr)
    ry[0].start()
    tx[0] = remote(tok_in.at[z], rows_out.at[me, :, xcols(x)], tx_send.at[0], tx_recv.at[0], x_nbr)
    tx[0].start()

    wsends = {}
    for n, k in enumerate(ks):
        pz, py = peer_of(k)
        p = pz * n_y + py
        if k != (0, 0):
            for i, (src, dst) in enumerate(((gate_in, gate_out), (up_in, up_out))):
                cp = remote(src.at[p], dst.at[0, grow(c, me)],
                            w_send.at[3 * n + i], w_recv.at[3 * n + i], dev(c, pz, py, x))
                cp.start()
                wsends[n, i] = cp
            cp = remote(down_in.at[p], down_out.at[0, drow(me), xcols(x)],
                        w_send.at[3 * n + 2], w_recv.at[3 * n + 2], dev(x, pz, py, c))
            cp.start()
            wsends[n, 2] = cp
        else:
            own_w = []
            for i, (src, dst) in enumerate(((gate_in, gate_out), (up_in, up_out))):
                cp = pltpu.make_async_copy(src.at[me], dst.at[0, grow(c, me)], own.at[2 + i])
                cp.start()
                own_w.append(cp)
                fw = remote(src.at[me], dst.at[0, grow(c, me)],
                            f_send.at[3 * n + i], f_recv.at[3 * n + i], other)
                fw.start()
                waits.append(fw)
            n_own = n
            own_down = pltpu.make_async_copy(
                down_in.at[me], down_out.at[0, drow(me), xcols(x)], own.at[4])
            far_down = remote(down_in.at[me], down_out.at[0, drow(me), xcols(x)],
                              w_send.at[3 * n + 2], w_recv.at[3 * n + 2], dev(x, z, y, c))

            @pl.when(c == x)
            def _():
                own_down.start()

            @pl.when(c != x)
            def _():
                far_down.start()

    for kz in (1, 2, 3):
        src = flip(z, kz) * n_y + y
        tz[kz].wait_recv()
        block = rows_out.at[src, :, xcols(x)]
        ty[kz] = remote(block, block, ty_send.at[kz], ty_recv.at[kz], y_nbr)
        ty[kz].start()
        tx[kz] = remote(block, block, tx_send.at[kz], tx_recv.at[kz], x_nbr)
        tx[kz].start()
        rz[kz].wait_recv()
        ry[kz] = remote(rw_out.at[src], rw_out.at[src], ry_send.at[kz], ry_recv.at[kz], y_nbr)
        ry[kz].start()
    for kz in (0, 1, 2, 3):
        src = flip(z, kz) * n_y + 1 - y
        ty[kz].wait_recv()
        block = rows_out.at[src, :, xcols(x)]
        tx[4 + kz] = remote(block, block, tx_send.at[4 + kz], tx_recv.at[4 + kz], x_nbr)
        tx[4 + kz].start()

    order = sorted(range(len(ks)), key=lambda n: (ks[n][0], ks[n][1]))
    for n in order:
        pz, py = peer_of(ks[n])
        p = pz * n_y + py
        if n != n_own:
            for i, dst in enumerate((gate_out, up_out)):
                wsends[n, i].wait_recv()
                block = dst.at[0, grow(c, p)]
                fw = remote(block, block, f_send.at[3 * n + i], f_recv.at[3 * n + i], other)
                fw.start()
                waits.append(fw)
            wsends[n, 2].wait_recv()
        else:

            @pl.when(c == x)
            def _():
                own_down.wait()

            @pl.when(c != x)
            def _():
                far_down.wait()

        block = down_out.at[0, drow(p), xcols(c)]
        fw = remote(block, block, f_send.at[3 * n + 2], f_recv.at[3 * n + 2], other)
        fw.start()
        waits.append(fw)

    for cp in own_w + [own_tok, own_rw]:
        cp.wait()
    for cp in list(wsends.values()) + list(tz.values()) + list(rz.values()) + list(ty.values()):
        cp.wait_send()
    for cp in list(ry.values()) + list(tx.values()) + waits:
        cp.wait()


def hand_back(
    n_z, n_y, p_in, ret_out,
    rx1, ry1, s0, s1, ry2, rx2, fin,
    a_send, a_recv, b_send, b_recv, z_send, z_recv, own,
):
    c, z, y, x = place(n_z, n_y)
    dev = functools.partial(device, n_y=n_y)
    x_nbr = dev(c, z, y, 1 - x)
    y_nbr = dev(c, z, 1 - y, x)
    greet([x_nbr, y_nbr] + [dev(c, flip(z, k), y, x) for k in (1, 2, 3)])
    half = p_in.shape[3] // 2
    q = half // 2

    def cols(i, j):
        return pl.ds(pl.multiple_of(i * half + j * q, q), q)

    def add(a, b):
        return (a.astype(jnp.float32) + b.astype(jnp.float32)).astype(BF16)

    first = {}
    for n, k in enumerate((3, 2, 1, 0)):
        zs = flip(z, k)
        moves = [
            (p_in.at[0, zs, :, cols(1 - x, 0)], rx1.at[n, 0], x_nbr),
            (p_in.at[1, zs, :, cols(1 - x, 0)], rx1.at[n, 1], x_nbr),
            (p_in.at[1 - y, zs, :, cols(0, 1)], ry1.at[n, 0], y_nbr),
            (p_in.at[1 - y, zs, :, cols(1, 1)], ry1.at[n, 1], y_nbr),
        ]
        for i, (src, dst, peer) in enumerate(moves):
            first[n, i] = remote(src, dst, a_send.at[4 * n + i], a_recv.at[4 * n + i], peer)
            first[n, i].start()
    second = {}
    for n, k in enumerate((3, 2, 1, 0)):
        zs = flip(z, k)
        for i in range(2):
            first[n, i].wait_recv()
            s0[n, i] = add(p_in[i, zs, :, cols(x, 0)], rx1[n, i])
        second[n, 0] = remote(s0.at[n, 1 - y], ry2.at[n], b_send.at[2 * n], b_recv.at[2 * n], y_nbr)
        second[n, 0].start()
        for i in range(2):
            first[n, 2 + i].wait_recv()
            s1[n, i] = add(p_in[y, zs, :, cols(i, 1)], ry1[n, i])
        second[n, 1] = remote(
            s1.at[n, 1 - x], rx2.at[n], b_send.at[2 * n + 1], b_recv.at[2 * n + 1], x_nbr)
        second[n, 1].start()
    last = []
    for n, k in enumerate((3, 2, 1, 0)):
        second[n, 0].wait_recv()
        fin[n, :, :q] = add(s0[n, y], ry2[n])
        second[n, 1].wait_recv()
        fin[n, :, q:] = add(s1[n, x], rx2[n])
        if k:
            cp = remote(fin.at[n], ret_out.at[z], z_send.at[n], z_recv.at[n],
                        dev(c, flip(z, k), y, x))
        else:
            cp = pltpu.make_async_copy(fin.at[n], ret_out.at[z], own)
        cp.start()
        last.append(cp)
    for cp in last:
        cp.wait()
    for cp in list(first.values()) + list(second.values()):
        cp.wait_send()


def paired(n_z, n_y, tokens, route_ids, route_weights, norm_gain, gate_weight, up_weight, down_weight):
    gate_folded = (gate_weight * norm_gain[None, :, None]).astype(BF16)
    up_folded = (up_weight * norm_gain[None, :, None]).astype(BF16)
    down_rounded = down_weight.astype(BF16)
    tok, width = tokens.shape
    experts = gate_weight.shape[0]
    epg = experts // GROUPS
    cap = tok // GROUPS
    half = width // lax.axis_size("tp")
    x = lax.axis_index("tp")
    n_fs = n_z * n_y

    group = route_ids[:, 0] // epg
    onehot = (group[:, None] == jnp.arange(GROUPS, dtype=jnp.int32)[None, :])
    before = jnp.arange(tok)[:, None] >= jnp.arange(tok)[None, :]
    upto = jnp.dot(before.astype(BF16), onehot.astype(BF16), preferred_element_type=jnp.float32)
    slot = jnp.sum(jnp.where(onehot, upto, 0.0), axis=1).astype(jnp.int32) - 1
    position = group * cap + slot
    pick = position[None, :] == jnp.arange(tok, dtype=jnp.int32)[:, None]
    pick_t = (position[:, None] == jnp.arange(tok, dtype=jnp.int32)[None, :]).astype(BF16)

    widened = tokens.astype(jnp.float32)
    scale = lax.rsqrt(jnp.mean(widened * widened, axis=-1, keepdims=True) + 1e-06)
    mine = lax.dynamic_slice_in_dim(tokens, x * half, half, axis=1)
    normed = (mine.astype(jnp.float32) * scale).astype(BF16)
    outgoing = jnp.dot(pick.astype(BF16), normed, preferred_element_type=jnp.float32)
    outgoing = outgoing.astype(BF16).reshape(GROUPS, cap, half)
    even = route_ids[:, 0] % epg == 0
    w_of = jnp.stack([
        jnp.where(even, route_weights[:, 0], route_weights[:, 1]),
        jnp.where(even, route_weights[:, 1], route_weights[:, 0]),
    ])
    w_sorted = jnp.sum(jnp.where(pick[None], w_of[:, None, :], 0.0), axis=2)
    w_sorted = w_sorted.reshape(2, GROUPS, cap).transpose(1, 0, 2)
    w_out = jnp.zeros((GROUPS, 8, -(-cap // 128) * 128), jnp.float32)
    w_out = lax.dynamic_update_slice(w_out, w_sorted, (0, 0, 0))

    hbm = pl.BlockSpec(memory_space=pl.ANY)
    vmem = pl.BlockSpec(memory_space=pltpu.VMEM)
    dma = pltpu.SemaphoreType.DMA
    d_rows, d_cols = down_weight.shape[1:]
    g_rows, g_cols = gate_weight.shape[1:]
    gate_new, up_new, down_new, rows, w_in = pl.pallas_call(
        functools.partial(hand_over, n_z, n_y),
        out_shape=(
            jax.ShapeDtypeStruct((1, 2 * n_fs * g_rows, g_cols), BF16),
            jax.ShapeDtypeStruct((1, 2 * n_fs * g_rows, g_cols), BF16),
            jax.ShapeDtypeStruct((1, n_fs * d_rows, 2 * d_cols), BF16),
            jax.ShapeDtypeStruct((n_fs, cap, width), BF16),
            jax.ShapeDtypeStruct((n_fs,) + w_out.shape[1:], jnp.float32),
        ),
        in_specs=[vmem] * 5,
        out_specs=(hbm,) * 5,
        scratch_shapes=[
            dma((3 * n_fs,)), dma((3 * n_fs,)), dma((3 * n_fs,)), dma((3 * n_fs,)),
            dma((4,)), dma((4,)), dma((4,)), dma((4,)), dma((8,)), dma((8,)),
            dma((4,)), dma((4,)), dma((4,)), dma((4,)), dma((5,)), dma((1,)),
        ],
        compiler_params=pltpu.CompilerParams(collective_id=0, has_side_effects=True),
    )(gate_folded, up_folded, down_rounded, outgoing, w_out)

    y = lax.rem(lax.axis_index("fs"), n_y)
    w_rows = lax.dynamic_index_in_dim(w_in, y, axis=1, keepdims=False)[:, :cap].reshape(n_fs * cap, 1)
    flat = rows.reshape(n_fs * cap, width)
    first = jnp.dot(flat, gate_new[0], preferred_element_type=jnp.float32)
    second = jnp.dot(flat, up_new[0], preferred_element_type=jnp.float32)
    hidden = (jax.nn.silu(first) * second).astype(BF16)
    part = jnp.dot(hidden, down_new[0], preferred_element_type=jnp.float32) * w_rows
    part = part.astype(BF16).reshape(n_z, n_y, cap, width).transpose(1, 0, 2, 3)

    q = half // 2
    ret = pl.pallas_call(
        functools.partial(hand_back, n_z, n_y),
        out_shape=jax.ShapeDtypeStruct((GROUPS, cap, half), BF16),
        in_specs=[vmem],
        out_specs=hbm,
        scratch_shapes=[
            pltpu.VMEM((4, 2, cap, q), BF16), pltpu.VMEM((4, 2, cap, q), BF16),
            pltpu.VMEM((4, 2, cap, q), BF16), pltpu.VMEM((4, 2, cap, q), BF16),
            pltpu.VMEM((4, cap, q), BF16), pltpu.VMEM((4, cap, q), BF16),
            pltpu.VMEM((4, cap, half), BF16),
            dma((16,)), dma((16,)), dma((8,)), dma((8,)), dma((4,)), dma((4,)), dma,
        ],
        compiler_params=pltpu.CompilerParams(collective_id=1, has_side_effects=True),
    )(part)
    mixed = jnp.dot(pick_t, ret.reshape(tok, half), preferred_element_type=jnp.float32)
    return gate_new, up_new, down_new, mixed.astype(BF16)


def solution(mesh):
    placed = (
        P(("gr", "fs"), None),
        P(("gr", "fs"), None),
        P(("gr", "fs"), None),
        P(("gr", "fs")),
        P(None, ("gr", "fs"), "tp"),
        P(None, ("gr", "fs"), "tp"),
        P(None, ("gr", "fs"), "tp"),
    )
    n_fs = mesh.shape["fs"]

    def body(*args):
        experts = args[4].shape[0]
        if experts == n_fs == 2 * GROUPS and mesh.shape["gr"] == mesh.shape["tp"] == 2:
            return paired(GROUPS, 2, *args)
        return local(*args)

    return jax.shard_map(
        body,
        mesh=mesh,
        in_specs=placed,
        out_specs=(
            P("fs", None, "tp"),
            P("fs", None, "tp"),
            P("fs", "tp", None),
            P(("gr", "fs"), "tp"),
        ),
        check_vma=False,
    )
```

```python
import functools

import jax
import jax.numpy as jnp
from jax import lax
from jax.experimental import pallas as pl
from jax.experimental.pallas import tpu as pltpu
from jax.sharding import PartitionSpec as P

GROUPS = 4
HEAD = 2
BF16 = jnp.bfloat16
MESH = pl.DeviceIdType.MESH


def local(tokens, route_ids, route_weights, norm_gain, gate_weight, up_weight, down_weight):
    gate_folded = (gate_weight * norm_gain[None, :, None]).astype(jnp.bfloat16)
    up_folded = (up_weight * norm_gain[None, :, None]).astype(jnp.bfloat16)
    down_rounded = down_weight.astype(jnp.bfloat16)
    moved = (
        lax.all_to_all(gate_folded, "fs", split_axis=0, concat_axis=1, tiled=True),
        lax.all_to_all(up_folded, "fs", split_axis=0, concat_axis=1, tiled=True),
        lax.all_to_all(down_rounded, "fs", split_axis=0, concat_axis=1, tiled=True),
    )
    gate_new, up_new, down_whole = (
        lax.all_gather(moved[0], "gr", axis=1, tiled=True),
        lax.all_gather(moved[1], "gr", axis=1, tiled=True),
        lax.all_gather(moved[2], "gr", axis=1, tiled=True),
    )
    down_new = lax.all_to_all(down_whole, "tp", split_axis=1, concat_axis=2, tiled=True)
    tok = tokens.shape[0]
    width = tokens.shape[1]
    experts = gate_weight.shape[0]
    cap = 2 * tok // experts
    flat_ids = route_ids.reshape(-1)
    onehot = (flat_ids[:, None] == jnp.arange(experts, dtype=jnp.int32)[None, :]).astype(jnp.int32)
    slot = jnp.sum(jnp.cumsum(onehot, axis=0) * onehot, axis=1) - 1
    position = flat_ids * cap + slot
    source = (
        jnp.zeros((experts * cap,), jnp.int32)
        .at[position]
        .set(jnp.arange(2 * tok, dtype=jnp.int32) // 2)
    )
    widened = tokens.astype(jnp.float32)
    normed = (
        widened * lax.rsqrt(jnp.mean(widened * widened, axis=-1, keepdims=True) + 1e-06)
    ).astype(jnp.bfloat16)
    outgoing = normed[source].reshape(experts, cap, width)
    received = lax.all_to_all(outgoing, "fs", split_axis=0, concat_axis=0, tiled=True)
    senders, count, _ = received.shape
    rows = received.reshape(senders * count, width)
    first = jnp.dot(rows, gate_new[0], preferred_element_type=jnp.float32)
    second = jnp.dot(rows, up_new[0], preferred_element_type=jnp.float32)
    hidden = (jax.nn.silu(first) * second).astype(jnp.bfloat16)
    partial_out = jnp.dot(hidden, down_new[0], preferred_element_type=jnp.float32)
    summed = lax.psum_scatter(
        partial_out.reshape(senders, count, width).astype(jnp.bfloat16),
        "tp",
        scatter_dimension=2,
        tiled=True,
    )
    returned = lax.all_to_all(summed, "fs", split_axis=0, concat_axis=0, tiled=True)
    columns = returned.shape[2]
    route_out = returned.reshape(experts * cap, columns)[position].reshape(tok, 2, columns)
    mixed = jnp.sum(route_weights[:, :, None] * route_out.astype(jnp.float32), axis=1).astype(
        jnp.bfloat16
    )
    return (gate_new, up_new, down_new, mixed)


def place(n_z, n_y):
    f = lax.axis_index("fs")
    return lax.axis_index("gr"), f // n_y, lax.rem(f, n_y), lax.axis_index("tp")


def flip(z, k):
    return (z, z + 1 - 2 * lax.rem(z, 2), lax.rem(z + 2, 4), 3 - z)[k]


def device(c, z, y, x, n_y):
    return {"gr": c, "fs": z * n_y + y, "tp": x}


def greet(peers):
    barrier = pltpu.get_barrier_semaphore()
    for peer in peers:
        pl.semaphore_signal(barrier, inc=1, device_id=peer, device_id_type=MESH)
    pl.semaphore_wait(barrier, len(peers))


def remote(src, dst, send, recv, peer):
    return pltpu.make_async_remote_copy(
        src_ref=src, dst_ref=dst, send_sem=send, recv_sem=recv,
        device_id=peer, device_id_type=MESH,
    )


def sampler(
    n_z, n_y,
    tok_in, group_in, rw_in, gain_in, gate_in, up_in, down_in,
    gate_out, up_out, down_out, mixed_out,
    wide, narrow, dwide, dnarrow, land, dland, dcross,
    normed, tok_s, rows, rw_s, rw_l, hid, out_s, ry_l, fin, ret,
    ld_sem, w_send, w_recv, f_send, f_recv,
    tz_send, tz_recv, ty_send, ty_recv, tx_send, tx_recv,
    rz_send, rz_recv, ry_send, ry_recv,
    h_send, h_recv, c_send, c_recv, y_send, y_recv, z_send, z_recv, o_sem,
):
    c, z, y, x = place(n_z, n_y)
    me = z * n_y + y
    n_fs = n_z * n_y
    g_rows, d_rows = gate_in.shape[1], down_in.shape[1]
    tok, width = tok_in.shape
    half = width // 2
    cap = tok // GROUPS
    hb = hid.shape[2]
    f32 = jnp.float32
    dev = functools.partial(device, n_y=n_y)
    ks = [(kz, ky) for kz in (3, 2, 1, 0) for ky in (1, 0)]
    last = len(ks) - 1
    at = []
    for kz, ky in ks:
        pz, py = flip(z, kz), (1 - y if ky else y)
        at.append((pz * n_y + py, dev(c, pz, py, x)))
    other = dev(1 - c, z, y, x)
    x_nbr = dev(c, z, y, 1 - x)
    y_nbr = dev(c, z, 1 - y, x)

    def xcols(i):
        return pl.ds(pl.multiple_of(i * half, half), half)

    def grow(core, f):
        return pl.ds(pl.multiple_of((core * n_fs + f) * g_rows, g_rows), g_rows)

    def drow(core, f):
        return pl.ds(pl.multiple_of((core * n_fs + f) * d_rows, d_rows), d_rows)

    def trow(f):
        return pl.ds(pl.multiple_of(f * cap, cap), cap)

    pair = (gate_in, up_in)
    loads = {}
    for n, (p, _) in enumerate(at):
        for i in range(2):
            loads[n, i] = pltpu.make_async_copy(pair[i].at[p], wide.at[i, n], ld_sem.at[3 * n + i])
            loads[n, i].start()
    for n, (p, _) in enumerate(at):
        loads[n, 2] = pltpu.make_async_copy(down_in.at[p], dwide.at[n], ld_sem.at[3 * n + 2])
        loads[n, 2].start()
    greet([d for _, d in at[:last]] + [other, x_nbr])

    def column(row, count):
        lanes = row.shape[1]
        eye = (lax.broadcasted_iota(jnp.int32, (count, lanes), 0)
               == lax.broadcasted_iota(jnp.int32, (count, lanes), 1))
        return jnp.sum(jnp.where(eye, row, 0.0), axis=1, keepdims=True)

    gain = column(gain_in[...], g_rows)
    sends = []
    arrive = {}
    onward = {}

    def fold(n):
        p, peer = at[n]
        for i in range(2):
            loads[n, i].wait()
            value = (wide[i, n] * gain).astype(BF16)
            if n == last:
                land[i, grow(c, me)] = value
                block = land.at[i, grow(c, me)]
                onward[n, i] = remote(block, block, f_send.at[3 * n + i], f_recv.at[3 * n + i], other)
                onward[n, i].start()
            else:
                narrow[i, n] = value
                cp = remote(narrow.at[i, n], land.at[i, grow(c, me)],
                            w_send.at[3 * n + i], w_recv.at[3 * n + i], peer)
                cp.start()
                arrive[n, i] = cp

    for n in range(HEAD):
        fold(n)

    def norm_rows(i, carry):
        r = pl.ds(pl.multiple_of(i * cap, cap), cap)
        v = tok_in[r, :].astype(f32)
        scale = lax.rsqrt(jnp.mean(v * v, axis=-1, keepdims=True) + 1e-06)
        normed[r, :] = (tok_in[r, xcols(x)].astype(f32) * scale).astype(BF16)
        return carry

    lax.fori_loop(0, GROUPS, norm_rows, 0)
    group = group_in[...]
    onehot = (lax.broadcasted_iota(jnp.int32, (8, tok), 0) == group).astype(f32)
    upto = (lax.broadcasted_iota(jnp.int32, (tok, tok), 0)
            <= lax.broadcasted_iota(jnp.int32, (tok, tok), 1)).astype(BF16)
    count = jnp.dot(onehot.astype(BF16), upto, preferred_element_type=f32)
    slot = jnp.sum(onehot * count, axis=0, keepdims=True).astype(jnp.int32) - 1
    position = group * cap + slot

    def picked(g):
        return lax.broadcasted_iota(jnp.int32, (cap, tok), 0) + g * cap == position

    tz, rz, ty, tx, ry = {}, {}, {}, {}, {}
    for kz in (3, 2, 1, 0):
        g = flip(z, kz)
        pick = picked(g)
        block = jnp.dot(pick.astype(BF16), normed[...], preferred_element_type=f32).astype(BF16)
        w_row = lax.dot_general(rw_in[...], pick.astype(f32), (((1,), (1,)), ((), ())),
                                precision=lax.Precision.HIGHEST, preferred_element_type=f32)
        if kz:
            tok_s[kz] = block
            rw_s[kz, :, :cap] = w_row
            peer = dev(c, g, y, x)
            tz[kz] = remote(tok_s.at[kz], rows.at[trow(me), xcols(x)],
                            tz_send.at[kz], tz_recv.at[kz], peer)
            tz[kz].start()
            rz[kz] = remote(rw_s.at[kz], rw_l.at[me], rz_send.at[kz], rz_recv.at[kz], peer)
            rz[kz].start()
        else:
            rows[trow(me), xcols(x)] = block
            rw_l[me, :, :cap] = w_row

    def pass_on(kz):
        src = flip(z, kz) * n_y + y
        block = rows.at[trow(src), xcols(x)]
        ty[kz] = remote(block, block, ty_send.at[kz], ty_recv.at[kz], y_nbr)
        ty[kz].start()
        tx[kz] = remote(block, block, tx_send.at[kz], tx_recv.at[kz], x_nbr)
        tx[kz].start()
        ry[kz] = remote(rw_l.at[src], rw_l.at[src], ry_send.at[kz], ry_recv.at[kz], y_nbr)
        ry[kz].start()

    pass_on(0)
    for n in range(HEAD, len(ks)):
        fold(n)
    for n, (p, peer) in enumerate(at):
        loads[n, 2].wait()
        value = dwide[n].astype(BF16)
        if n == last:
            dland[drow(c, me)] = value
            block = dland.at[drow(c, me)]
            onward[n, 2] = remote(block, block, f_send.at[3 * n + 2], f_recv.at[3 * n + 2], other)
            onward[n, 2].start()
        else:
            dnarrow[n] = value
            arrive[n, 2] = remote(dnarrow.at[n], dland.at[drow(c, me)],
                                  w_send.at[3 * n + 2], w_recv.at[3 * n + 2], peer)
            arrive[n, 2].start()

    for kz in (1, 2, 3):
        tz[kz].wait_recv()
        rz[kz].wait_recv()
        pass_on(kz)
    for kz in (0, 1, 2, 3):
        ty[kz].wait_recv()
        block = rows.at[trow(flip(z, kz) * n_y + 1 - y), xcols(x)]
        tx[4 + kz] = remote(block, block, tx_send.at[4 + kz], tx_recv.at[4 + kz], x_nbr)
        tx[4 + kz].start()

    order = sorted(range(last), key=lambda n: ks[n])
    for n in order:
        for i in range(2):
            arrive[n, i].wait_recv()
            block = land.at[i, grow(c, at[n][0])]
            onward[n, i] = remote(block, block, f_send.at[3 * n + i], f_recv.at[3 * n + i], other)
            onward[n, i].start()
    for cp in list(tx.values()) + list(ry.values()):
        cp.wait_recv()
    for n in [last] + order:
        for i in range(2):
            onward[n, i].wait_recv()
    outs = []
    for i, out in enumerate((gate_out, up_out)):
        cp = pltpu.make_async_copy(land.at[i], out.at[0], o_sem.at[i])
        cp.start()
        outs.append(cp)

    m, q = rows.shape[0] // 2, 256
    hsend = []
    for j in range(2):
        r = pl.ds(j * m, m)

        def units(i, carry):
            s = pl.ds(pl.multiple_of(i * q, q), q)
            a = jnp.dot(rows[r, :], land[0, :, s], preferred_element_type=f32)
            b = jnp.dot(rows[r, :], land[1, :, s], preferred_element_type=f32)
            hid[x, r, s] = (a / (1.0 + jnp.exp(-a)) * b).astype(BF16)
            return carry

        lax.fori_loop(0, hb // q, units, 0)
        cp = remote(hid.at[x, r], hid.at[x, r], h_send.at[j], h_recv.at[j], x_nbr)
        cp.start()
        hsend.append(cp)

    for n in order:
        arrive[n, 2].wait_recv()
        block = dland.at[drow(c, at[n][0])]
        onward[n, 2] = remote(block, block, f_send.at[3 * n + 2], f_recv.at[3 * n + 2], other)
        onward[n, 2].start()
    for n in [last] + order:
        onward[n, 2].wait_recv()
    for cp in hsend:
        cp.wait_recv()
    part = hb // 2
    mine = pl.ds(pl.multiple_of(c * part, part), part)
    cross = remote(
        dland.at[pl.ds(pl.multiple_of((1 - x) * hb + c * part, part), part)],
        dcross.at[mine], c_send.at[0], c_recv.at[0], x_nbr)
    cross.start()
    cp = pltpu.make_async_copy(
        dland.at[pl.ds(pl.multiple_of(x * hb, hb), hb)], down_out.at[0, :, xcols(x)], o_sem.at[2])
    cp.start()
    outs.append(cp)

    ysend = []
    for n, kz in enumerate((3, 2, 1, 0)):
        zs = flip(z, kz)
        for step in range(2):
            s = 1 - y if step == 0 else y
            f = zs * n_y + s
            acc = jnp.dot(hid[0, trow(f)], dland[:hb], preferred_element_type=f32)
            acc += jnp.dot(hid[1, trow(f)], dland[hb:], preferred_element_type=f32)
            w = jnp.where(y == 0, rw_l[f, 0:1, :], rw_l[f, 1:2, :])
            lane = lax.broadcasted_iota(jnp.int32, w.shape, 1)
            w = jnp.where(lane < cap, w, 0.0)
            out_s[n, step] = (acc * column(w, cap)).astype(BF16)
            if step == 0:
                cp = remote(out_s.at[n, 0], ry_l.at[n], y_send.at[n], y_recv.at[n], y_nbr)
                cp.start()
                ysend.append(cp)
    zsend = []
    for n, kz in enumerate((3, 2, 1, 0)):
        ysend[n].wait_recv()
        total = (out_s[n, 1].astype(f32) + ry_l[n].astype(f32)).astype(BF16)
        if kz:
            fin[n] = total
            cp = remote(fin.at[n], ret.at[trow(z)], z_send.at[n], z_recv.at[n],
                        dev(c, flip(z, kz), y, x))
            cp.start()
            zsend.append(cp)
        else:
            ret[trow(z)] = total

    cross.wait_recv()
    over = remote(dcross.at[mine], dcross.at[mine], c_send.at[1], c_recv.at[1], other)
    over.start()
    for cp in zsend:
        cp.wait_recv()
    everyone = (lax.broadcasted_iota(jnp.int32, (tok, tok), 0) == position).astype(BF16)
    mixed_out[...] = lax.dot_general(
        everyone, ret[...], (((0,), (0,)), ((), ())), preferred_element_type=f32).astype(BF16)
    over.wait_recv()
    cp = pltpu.make_async_copy(dcross, down_out.at[0, :, xcols(1 - x)], o_sem.at[3])
    cp.start()
    outs.append(cp)
    for cp in outs:
        cp.wait()
    for group_of in (arrive, onward, tz, rz, ty, tx, ry):
        for cp in group_of.values():
            cp.wait_send()
    for cp in hsend + ysend + zsend + [cross, over]:
        cp.wait_send()


def paired(n_z, n_y, tokens, route_ids, route_weights, norm_gain, gate_weight, up_weight, down_weight):
    tok, width = tokens.shape
    experts = gate_weight.shape[0]
    epg = experts // GROUPS
    cap = tok // GROUPS
    half = width // lax.axis_size("tp")
    n_fs = n_z * n_y
    d_rows, d_cols = down_weight.shape[1:]
    g_rows, g_cols = gate_weight.shape[1:]
    f32 = jnp.float32

    group = (route_ids[:, 0] // epg).reshape(1, tok)
    even = route_ids[:, 0] % epg == 0
    w_first, w_second = route_weights[:, 0], route_weights[:, 1]
    w_of = jnp.stack([jnp.where(even, w_first, w_second), jnp.where(even, w_second, w_first)])
    w_of = jnp.pad(w_of, ((0, 6), (0, 0)))

    hbm = pl.BlockSpec(memory_space=pl.ANY)
    vmem = pl.BlockSpec(memory_space=pltpu.VMEM)
    dma = pltpu.SemaphoreType.DMA
    lanes = -(-cap // 128) * 128
    gate_new, up_new, down_new, mixed = pl.pallas_call(
        functools.partial(sampler, n_z, n_y),
        out_shape=(
            jax.ShapeDtypeStruct((1, 2 * n_fs * g_rows, g_cols), BF16),
            jax.ShapeDtypeStruct((1, 2 * n_fs * g_rows, g_cols), BF16),
            jax.ShapeDtypeStruct((1, n_fs * d_rows, 2 * d_cols), BF16),
            jax.ShapeDtypeStruct((tok, half), BF16),
        ),
        in_specs=[vmem] * 4 + [hbm] * 3,
        out_specs=(hbm, hbm, hbm, vmem),
        scratch_shapes=[
            pltpu.VMEM((2, n_fs, g_rows, g_cols), f32),
            pltpu.VMEM((2, n_fs - 1, g_rows, g_cols), BF16),
            pltpu.VMEM((n_fs, d_rows, d_cols), f32),
            pltpu.VMEM((n_fs - 1, d_rows, d_cols), BF16),
            pltpu.VMEM((2, 2 * n_fs * g_rows, g_cols), BF16),
            pltpu.VMEM((2 * n_fs * d_rows, d_cols), BF16),
            pltpu.VMEM((n_fs * d_rows, d_cols), BF16),
            pltpu.VMEM((tok, half), BF16),
            pltpu.VMEM((4, cap, half), BF16),
            pltpu.VMEM((n_fs * cap, width), BF16),
            pltpu.VMEM((4, 8, lanes), f32),
            pltpu.VMEM((n_fs, 8, lanes), f32),
            pltpu.VMEM((2, n_fs * cap, n_fs * d_rows), BF16),
            pltpu.VMEM((4, 2, cap, half), BF16),
            pltpu.VMEM((4, cap, half), BF16),
            pltpu.VMEM((4, cap, half), BF16),
            pltpu.VMEM((GROUPS * cap, half), BF16),
            dma((3 * n_fs,)),
            dma((3 * n_fs,)), dma((3 * n_fs,)), dma((3 * n_fs,)), dma((3 * n_fs,)),
            dma((4,)), dma((4,)), dma((4,)), dma((4,)), dma((8,)), dma((8,)),
            dma((4,)), dma((4,)), dma((4,)), dma((4,)),
            dma((2,)), dma((2,)), dma((2,)), dma((2,)), dma((4,)), dma((4,)),
            dma((4,)), dma((4,)), dma((4,)),
        ],
        compiler_params=pltpu.CompilerParams(
            collective_id=0, has_side_effects=True, vmem_limit_bytes=56 * 1024 * 1024),
    )(tokens, group, w_of, norm_gain.reshape(1, g_rows), gate_weight, up_weight, down_weight)
    return gate_new, up_new, down_new, mixed


def solution(mesh):
    placed = (
        P(("gr", "fs"), None),
        P(("gr", "fs"), None),
        P(("gr", "fs"), None),
        P(("gr", "fs")),
        P(None, ("gr", "fs"), "tp"),
        P(None, ("gr", "fs"), "tp"),
        P(None, ("gr", "fs"), "tp"),
    )
    n_fs = mesh.shape["fs"]

    def body(*args):
        experts = args[4].shape[0]
        if experts == n_fs == 2 * GROUPS and mesh.shape["gr"] == mesh.shape["tp"] == 2:
            return paired(GROUPS, 2, *args)
        return local(*args)

    return jax.shard_map(
        body,
        mesh=mesh,
        in_specs=placed,
        out_specs=(
            P("fs", None, "tp"),
            P("fs", None, "tp"),
            P("fs", "tp", None),
            P(("gr", "fs"), "tp"),
        ),
        check_vma=False,
    )
```

```python
import functools

import jax
import jax.numpy as jnp
from jax import lax
from jax.experimental import pallas as pl
from jax.experimental.pallas import tpu as pltpu
from jax.sharding import PartitionSpec as P

GROUPS = 4
HEAD = 2
BF16 = jnp.bfloat16
MESH = pl.DeviceIdType.MESH


def local(tokens, route_ids, route_weights, norm_gain, gate_weight, up_weight, down_weight):
    gate_folded = (gate_weight * norm_gain[None, :, None]).astype(jnp.bfloat16)
    up_folded = (up_weight * norm_gain[None, :, None]).astype(jnp.bfloat16)
    down_rounded = down_weight.astype(jnp.bfloat16)
    moved = (
        lax.all_to_all(gate_folded, "fs", split_axis=0, concat_axis=1, tiled=True),
        lax.all_to_all(up_folded, "fs", split_axis=0, concat_axis=1, tiled=True),
        lax.all_to_all(down_rounded, "fs", split_axis=0, concat_axis=1, tiled=True),
    )
    gate_new, up_new, down_whole = (
        lax.all_gather(moved[0], "gr", axis=1, tiled=True),
        lax.all_gather(moved[1], "gr", axis=1, tiled=True),
        lax.all_gather(moved[2], "gr", axis=1, tiled=True),
    )
    down_new = lax.all_to_all(down_whole, "tp", split_axis=1, concat_axis=2, tiled=True)
    tok = tokens.shape[0]
    width = tokens.shape[1]
    experts = gate_weight.shape[0]
    cap = 2 * tok // experts
    flat_ids = route_ids.reshape(-1)
    onehot = (flat_ids[:, None] == jnp.arange(experts, dtype=jnp.int32)[None, :]).astype(jnp.int32)
    slot = jnp.sum(jnp.cumsum(onehot, axis=0) * onehot, axis=1) - 1
    position = flat_ids * cap + slot
    source = (
        jnp.zeros((experts * cap,), jnp.int32)
        .at[position]
        .set(jnp.arange(2 * tok, dtype=jnp.int32) // 2)
    )
    widened = tokens.astype(jnp.float32)
    normed = (
        widened * lax.rsqrt(jnp.mean(widened * widened, axis=-1, keepdims=True) + 1e-06)
    ).astype(jnp.bfloat16)
    outgoing = normed[source].reshape(experts, cap, width)
    received = lax.all_to_all(outgoing, "fs", split_axis=0, concat_axis=0, tiled=True)
    senders, count, _ = received.shape
    rows = received.reshape(senders * count, width)
    first = jnp.dot(rows, gate_new[0], preferred_element_type=jnp.float32)
    second = jnp.dot(rows, up_new[0], preferred_element_type=jnp.float32)
    hidden = (jax.nn.silu(first) * second).astype(jnp.bfloat16)
    partial_out = jnp.dot(hidden, down_new[0], preferred_element_type=jnp.float32)
    summed = lax.psum_scatter(
        partial_out.reshape(senders, count, width).astype(jnp.bfloat16),
        "tp",
        scatter_dimension=2,
        tiled=True,
    )
    returned = lax.all_to_all(summed, "fs", split_axis=0, concat_axis=0, tiled=True)
    columns = returned.shape[2]
    route_out = returned.reshape(experts * cap, columns)[position].reshape(tok, 2, columns)
    mixed = jnp.sum(route_weights[:, :, None] * route_out.astype(jnp.float32), axis=1).astype(
        jnp.bfloat16
    )
    return (gate_new, up_new, down_new, mixed)


def place(n_z, n_y):
    f = lax.axis_index("fs")
    return lax.axis_index("gr"), f // n_y, lax.rem(f, n_y), lax.axis_index("tp")


def flip(z, k):
    return (z, z + 1 - 2 * lax.rem(z, 2), lax.rem(z + 2, 4), 3 - z)[k]


def device(c, z, y, x, n_y):
    return {"gr": c, "fs": z * n_y + y, "tp": x}


def greet(peers):
    barrier = pltpu.get_barrier_semaphore()
    for peer in peers:
        pl.semaphore_signal(barrier, inc=1, device_id=peer, device_id_type=MESH)
    pl.semaphore_wait(barrier, len(peers))


def remote(src, dst, send, recv, peer):
    return pltpu.make_async_remote_copy(
        src_ref=src, dst_ref=dst, send_sem=send, recv_sem=recv,
        device_id=peer, device_id_type=MESH,
    )


def sampler(
    n_z, n_y,
    tok_in, ids_in, rw_in, gain_in, gate_in, up_in, down_in,
    gate_out, up_out, down_out, mixed_out,
    wide, narrow, dwide, dnarrow, land, dland, dcross,
    normed, tok_s, rows, rw_s, rw_l, hid, out_s, ry_l, fin, ret,
    ld_sem, w_send, w_recv, f_send, f_recv,
    tz_send, tz_recv, ty_send, ty_recv, tx_send, tx_recv,
    rz_send, rz_recv, ry_send, ry_recv,
    h_send, h_recv, c_send, c_recv, y_send, y_recv, z_send, z_recv, o_sem,
):
    c, z, y, x = place(n_z, n_y)
    me = z * n_y + y
    n_fs = n_z * n_y
    g_rows, d_rows = gate_in.shape[1], down_in.shape[1]
    tok, width = tok_in.shape
    half = width // 2
    cap = tok // GROUPS
    hb = hid.shape[2]
    f32 = jnp.float32
    dev = functools.partial(device, n_y=n_y)
    ks = [(kz, ky) for kz in (1, 3, 2, 0) for ky in (1, 0)]
    last = len(ks) - 1
    at = []
    for kz, ky in ks:
        pz, py = flip(z, kz), (1 - y if ky else y)
        at.append((pz * n_y + py, dev(c, pz, py, x)))
    other = dev(1 - c, z, y, x)
    x_nbr = dev(c, z, y, 1 - x)
    y_nbr = dev(c, z, 1 - y, x)

    def xcols(i):
        return pl.ds(pl.multiple_of(i * half, half), half)

    def grow(core, f):
        return pl.ds(pl.multiple_of((core * n_fs + f) * g_rows, g_rows), g_rows)

    def drow(core, f):
        return pl.ds(pl.multiple_of((core * n_fs + f) * d_rows, d_rows), d_rows)

    def trow(f):
        return pl.ds(pl.multiple_of(f * cap, cap), cap)

    pair = (gate_in, up_in)
    loads = {}
    for n, (p, _) in enumerate(at):
        for i in range(2):
            loads[n, i] = pltpu.make_async_copy(pair[i].at[p], wide.at[i, n], ld_sem.at[3 * n + i])
            loads[n, i].start()
    for n, (p, _) in enumerate(at):
        loads[n, 2] = pltpu.make_async_copy(down_in.at[p], dwide.at[n], ld_sem.at[3 * n + 2])
        loads[n, 2].start()
    greet([d for _, d in at[:last]] + [other, x_nbr])

    def column(row, count):
        lanes = row.shape[1]
        eye = (lax.broadcasted_iota(jnp.int32, (count, lanes), 0)
               == lax.broadcasted_iota(jnp.int32, (count, lanes), 1))
        return jnp.sum(jnp.where(eye, row, 0.0), axis=1, keepdims=True)

    gain = column(gain_in[...], g_rows)
    arrive = {}
    onward = {}

    def fold(n):
        p, peer = at[n]
        for i in range(2):
            loads[n, i].wait()
            value = (wide[i, n] * gain).astype(BF16)
            if n == last:
                land[i, grow(c, me)] = value
                block = land.at[i, grow(c, me)]
                onward[n, i] = remote(block, block, f_send.at[3 * n + i], f_recv.at[3 * n + i], other)
                onward[n, i].start()
            else:
                narrow[i, n] = value
                cp = remote(narrow.at[i, n], land.at[i, grow(c, me)],
                            w_send.at[3 * n + i], w_recv.at[3 * n + i], peer)
                cp.start()
                arrive[n, i] = cp

    for n in range(HEAD):
        fold(n)

    def norm_rows(i, carry):
        r = pl.ds(pl.multiple_of(i * cap, cap), cap)
        v = tok_in[r, :].astype(f32)
        scale = lax.rsqrt(jnp.mean(v * v, axis=-1, keepdims=True) + 1e-06)
        normed[r, :] = (tok_in[r, xcols(x)].astype(f32) * scale).astype(BF16)
        return carry

    lax.fori_loop(0, GROUPS, norm_rows, 0)
    epg = gate_in.shape[0] // GROUPS
    low = ids_in[0:1, :]
    group = jnp.zeros_like(low)
    for g in range(1, GROUPS):
        group += (low >= g * epg).astype(jnp.int32)
    ahead = low == group * epg
    w_a, w_b = rw_in[0:1, :], rw_in[1:2, :]
    sub = lax.broadcasted_iota(jnp.int32, (8, tok), 0)
    w_of = jnp.where(sub == 0, jnp.where(ahead, w_a, w_b),
                     jnp.where(sub == 1, jnp.where(ahead, w_b, w_a), 0.0))
    onehot = (lax.broadcasted_iota(jnp.int32, (8, tok), 0) == group).astype(f32)
    upto = (lax.broadcasted_iota(jnp.int32, (tok, tok), 0)
            <= lax.broadcasted_iota(jnp.int32, (tok, tok), 1)).astype(BF16)
    count = jnp.dot(onehot.astype(BF16), upto, preferred_element_type=f32)
    slot = jnp.sum(onehot * count, axis=0, keepdims=True).astype(jnp.int32) - 1
    position = group * cap + slot

    def picked(g):
        return lax.broadcasted_iota(jnp.int32, (cap, tok), 0) + g * cap == position

    tz, rz, ty, tx, ry = {}, {}, {}, {}, {}
    for kz in (1, 3, 2, 0):
        g = flip(z, kz)
        pick = picked(g)
        block = jnp.dot(pick.astype(BF16), normed[...], preferred_element_type=f32).astype(BF16)
        w_row = lax.dot_general(w_of, pick.astype(f32), (((1,), (1,)), ((), ())),
                                precision=lax.Precision.HIGHEST, preferred_element_type=f32)
        if kz:
            tok_s[kz] = block
            rw_s[kz, :, :cap] = w_row
            peer = dev(c, g, y, x)
            tz[kz] = remote(tok_s.at[kz], rows.at[trow(me), xcols(x)],
                            tz_send.at[kz], tz_recv.at[kz], peer)
            tz[kz].start()
            rz[kz] = remote(rw_s.at[kz], rw_l.at[me], rz_send.at[kz], rz_recv.at[kz], peer)
            rz[kz].start()
        else:
            rows[trow(me), xcols(x)] = block
            rw_l[me, :, :cap] = w_row

    def pass_on(kz):
        src = flip(z, kz) * n_y + y
        block = rows.at[trow(src), xcols(x)]
        ty[kz] = remote(block, block, ty_send.at[kz], ty_recv.at[kz], y_nbr)
        ty[kz].start()
        tx[kz] = remote(block, block, tx_send.at[kz], tx_recv.at[kz], x_nbr)
        tx[kz].start()
        ry[kz] = remote(rw_l.at[src], rw_l.at[src], ry_send.at[kz], ry_recv.at[kz], y_nbr)
        ry[kz].start()

    pass_on(0)
    for n in range(HEAD, len(ks)):
        fold(n)
    for n, (p, peer) in enumerate(at):
        loads[n, 2].wait()
        value = dwide[n].astype(BF16)
        if n == last:
            dland[drow(c, me)] = value
            block = dland.at[drow(c, me)]
            onward[n, 2] = remote(block, block, f_send.at[3 * n + 2], f_recv.at[3 * n + 2], other)
            onward[n, 2].start()
        else:
            dnarrow[n] = value
            arrive[n, 2] = remote(dnarrow.at[n], dland.at[drow(c, me)],
                                  w_send.at[3 * n + 2], w_recv.at[3 * n + 2], peer)
            arrive[n, 2].start()

    for kz in (1, 2, 3):
        tz[kz].wait_recv()
        rz[kz].wait_recv()
        pass_on(kz)
    for kz in (0, 1, 2, 3):
        ty[kz].wait_recv()
        block = rows.at[trow(flip(z, kz) * n_y + 1 - y), xcols(x)]
        tx[4 + kz] = remote(block, block, tx_send.at[4 + kz], tx_recv.at[4 + kz], x_nbr)
        tx[4 + kz].start()

    order = sorted(range(last), key=lambda n: ks[n])
    for n in order:
        for i in range(2):
            arrive[n, i].wait_recv()
            block = land.at[i, grow(c, at[n][0])]
            onward[n, i] = remote(block, block, f_send.at[3 * n + i], f_recv.at[3 * n + i], other)
            onward[n, i].start()
    for cp in list(tx.values()) + list(ry.values()):
        cp.wait_recv()
    for n in [last] + order:
        for i in range(2):
            onward[n, i].wait_recv()
    outs = []
    for i, out in enumerate((gate_out, up_out)):
        cp = pltpu.make_async_copy(land.at[i], out.at[0], o_sem.at[i])
        cp.start()
        outs.append(cp)

    m, q = rows.shape[0] // 2, 256
    hsend = []
    for j in range(2):
        r = pl.ds(j * m, m)

        def units(i, carry):
            s = pl.ds(pl.multiple_of(i * q, q), q)
            a = jnp.dot(rows[r, :], land[0, :, s], preferred_element_type=f32)
            b = jnp.dot(rows[r, :], land[1, :, s], preferred_element_type=f32)
            hid[x, r, s] = (a / (1.0 + jnp.exp(-a)) * b).astype(BF16)
            return carry

        lax.fori_loop(0, hb // q, units, 0)
        cp = remote(hid.at[x, r], hid.at[x, r], h_send.at[j], h_recv.at[j], x_nbr)
        cp.start()
        hsend.append(cp)

    for n in order:
        arrive[n, 2].wait_recv()
        block = dland.at[drow(c, at[n][0])]
        onward[n, 2] = remote(block, block, f_send.at[3 * n + 2], f_recv.at[3 * n + 2], other)
        onward[n, 2].start()
    for n in [last] + order:
        onward[n, 2].wait_recv()
    for cp in hsend:
        cp.wait_recv()
    part = hb // 2
    mine = pl.ds(pl.multiple_of(c * part, part), part)
    cross = remote(
        dland.at[pl.ds(pl.multiple_of((1 - x) * hb + c * part, part), part)],
        dcross.at[mine], c_send.at[0], c_recv.at[0], x_nbr)
    cross.start()
    cp = pltpu.make_async_copy(
        dland.at[pl.ds(pl.multiple_of(x * hb, hb), hb)], down_out.at[0, :, xcols(x)], o_sem.at[2])
    cp.start()
    outs.append(cp)

    ysend = []
    for n, kz in enumerate((3, 1, 2, 0)):
        zs = flip(z, kz)
        for step in range(2):
            s = 1 - y if step == 0 else y
            f = zs * n_y + s
            acc = jnp.dot(hid[0, trow(f)], dland[:hb], preferred_element_type=f32)
            acc += jnp.dot(hid[1, trow(f)], dland[hb:], preferred_element_type=f32)
            w = jnp.where(y == 0, rw_l[f, 0:1, :], rw_l[f, 1:2, :])
            lane = lax.broadcasted_iota(jnp.int32, w.shape, 1)
            w = jnp.where(lane < cap, w, 0.0)
            out_s[n, step] = (acc * column(w, cap)).astype(BF16)
            if step == 0:
                cp = remote(out_s.at[n, 0], ry_l.at[n], y_send.at[n], y_recv.at[n], y_nbr)
                cp.start()
                ysend.append(cp)
    zsend = []
    for n, kz in enumerate((3, 1, 2, 0)):
        ysend[n].wait_recv()
        total = (out_s[n, 1].astype(f32) + ry_l[n].astype(f32)).astype(BF16)
        if kz:
            fin[n] = total
            cp = remote(fin.at[n], ret.at[trow(z)], z_send.at[n], z_recv.at[n],
                        dev(c, flip(z, kz), y, x))
            cp.start()
            zsend.append(cp)
        else:
            ret[trow(z)] = total

    cross.wait_recv()
    over = remote(dcross.at[mine], dcross.at[mine], c_send.at[1], c_recv.at[1], other)
    over.start()
    for cp in zsend:
        cp.wait_recv()
    everyone = (lax.broadcasted_iota(jnp.int32, (tok, tok), 0) == position).astype(BF16)
    mixed_out[...] = lax.dot_general(
        everyone, ret[...], (((0,), (0,)), ((), ())), preferred_element_type=f32).astype(BF16)
    over.wait_recv()
    cp = pltpu.make_async_copy(dcross, down_out.at[0, :, xcols(1 - x)], o_sem.at[3])
    cp.start()
    outs.append(cp)
    for cp in outs:
        cp.wait()
    for group_of in (arrive, onward, tz, rz, ty, tx, ry):
        for cp in group_of.values():
            cp.wait_send()
    for cp in hsend + ysend + zsend + [cross, over]:
        cp.wait_send()


def paired(n_z, n_y, tokens, route_ids, route_weights, norm_gain, gate_weight, up_weight, down_weight):
    tok, width = tokens.shape
    cap = tok // GROUPS
    half = width // lax.axis_size("tp")
    n_fs = n_z * n_y
    d_rows, d_cols = down_weight.shape[1:]
    g_rows, g_cols = gate_weight.shape[1:]
    f32 = jnp.float32

    hbm = pl.BlockSpec(memory_space=pl.ANY)
    vmem = pl.BlockSpec(memory_space=pltpu.VMEM)
    dma = pltpu.SemaphoreType.DMA
    lanes = -(-cap // 128) * 128
    gate_new, up_new, down_new, mixed = pl.pallas_call(
        functools.partial(sampler, n_z, n_y),
        out_shape=(
            jax.ShapeDtypeStruct((1, 2 * n_fs * g_rows, g_cols), BF16),
            jax.ShapeDtypeStruct((1, 2 * n_fs * g_rows, g_cols), BF16),
            jax.ShapeDtypeStruct((1, n_fs * d_rows, 2 * d_cols), BF16),
            jax.ShapeDtypeStruct((tok, half), BF16),
        ),
        in_specs=[vmem] * 4 + [pl.BlockSpec(memory_space=pltpu.HBM)] * 3,
        out_specs=(hbm, hbm, hbm, vmem),
        scratch_shapes=[
            pltpu.VMEM((2, n_fs, g_rows, g_cols), f32),
            pltpu.VMEM((2, n_fs - 1, g_rows, g_cols), BF16),
            pltpu.VMEM((n_fs, d_rows, d_cols), f32),
            pltpu.VMEM((n_fs - 1, d_rows, d_cols), BF16),
            pltpu.VMEM((2, 2 * n_fs * g_rows, g_cols), BF16),
            pltpu.VMEM((2 * n_fs * d_rows, d_cols), BF16),
            pltpu.VMEM((n_fs * d_rows, d_cols), BF16),
            pltpu.VMEM((tok, half), BF16),
            pltpu.VMEM((4, cap, half), BF16),
            pltpu.VMEM((n_fs * cap, width), BF16),
            pltpu.VMEM((4, 8, lanes), f32),
            pltpu.VMEM((n_fs, 8, lanes), f32),
            pltpu.VMEM((2, n_fs * cap, n_fs * d_rows), BF16),
            pltpu.VMEM((4, 2, cap, half), BF16),
            pltpu.VMEM((4, cap, half), BF16),
            pltpu.VMEM((4, cap, half), BF16),
            pltpu.VMEM((GROUPS * cap, half), BF16),
            dma((3 * n_fs,)),
            dma((3 * n_fs,)), dma((3 * n_fs,)), dma((3 * n_fs,)), dma((3 * n_fs,)),
            dma((4,)), dma((4,)), dma((4,)), dma((4,)), dma((8,)), dma((8,)),
            dma((4,)), dma((4,)), dma((4,)), dma((4,)),
            dma((2,)), dma((2,)), dma((2,)), dma((2,)), dma((4,)), dma((4,)),
            dma((4,)), dma((4,)), dma((4,)),
        ],
        compiler_params=pltpu.CompilerParams(
            collective_id=0, has_side_effects=True, vmem_limit_bytes=36 * 1024 * 1024),
    )(tokens, route_ids.T, route_weights.T, norm_gain.reshape(1, g_rows), gate_weight, up_weight, down_weight)
    return gate_new, up_new, down_new, mixed


def solution(mesh):
    placed = (
        P(("gr", "fs"), None),
        P(("gr", "fs"), None),
        P(("gr", "fs"), None),
        P(("gr", "fs")),
        P(None, ("gr", "fs"), "tp"),
        P(None, ("gr", "fs"), "tp"),
        P(None, ("gr", "fs"), "tp"),
    )
    n_fs = mesh.shape["fs"]

    def body(*args):
        experts = args[4].shape[0]
        if experts == n_fs == 2 * GROUPS and mesh.shape["gr"] == mesh.shape["tp"] == 2:
            return paired(GROUPS, 2, *args)
        return local(*args)

    return jax.shard_map(
        body,
        mesh=mesh,
        in_specs=placed,
        out_specs=(
            P("fs", None, "tp"),
            P("fs", None, "tp"),
            P("fs", "tp", None),
            P(("gr", "fs"), "tp"),
        ),
        check_vma=False,
    )
```

```python
import functools

import jax
import jax.numpy as jnp
from jax import lax
from jax.experimental import pallas as pl
from jax.experimental.pallas import tpu as pltpu
from jax.sharding import PartitionSpec as P

GROUPS = 4
HEAD = 2
MID = 3
PIECES = 2
RETURN = (3, 1, 2, 0)
BF16 = jnp.bfloat16
MESH = pl.DeviceIdType.MESH


def local(tokens, route_ids, route_weights, norm_gain, gate_weight, up_weight, down_weight):
    gate_folded = (gate_weight * norm_gain[None, :, None]).astype(jnp.bfloat16)
    up_folded = (up_weight * norm_gain[None, :, None]).astype(jnp.bfloat16)
    down_rounded = down_weight.astype(jnp.bfloat16)
    moved = (
        lax.all_to_all(gate_folded, "fs", split_axis=0, concat_axis=1, tiled=True),
        lax.all_to_all(up_folded, "fs", split_axis=0, concat_axis=1, tiled=True),
        lax.all_to_all(down_rounded, "fs", split_axis=0, concat_axis=1, tiled=True),
    )
    gate_new, up_new, down_whole = (
        lax.all_gather(moved[0], "gr", axis=1, tiled=True),
        lax.all_gather(moved[1], "gr", axis=1, tiled=True),
        lax.all_gather(moved[2], "gr", axis=1, tiled=True),
    )
    down_new = lax.all_to_all(down_whole, "tp", split_axis=1, concat_axis=2, tiled=True)
    tok = tokens.shape[0]
    width = tokens.shape[1]
    experts = gate_weight.shape[0]
    cap = 2 * tok // experts
    flat_ids = route_ids.reshape(-1)
    onehot = (flat_ids[:, None] == jnp.arange(experts, dtype=jnp.int32)[None, :]).astype(jnp.int32)
    slot = jnp.sum(jnp.cumsum(onehot, axis=0) * onehot, axis=1) - 1
    position = flat_ids * cap + slot
    source = (
        jnp.zeros((experts * cap,), jnp.int32)
        .at[position]
        .set(jnp.arange(2 * tok, dtype=jnp.int32) // 2)
    )
    widened = tokens.astype(jnp.float32)
    normed = (
        widened * lax.rsqrt(jnp.mean(widened * widened, axis=-1, keepdims=True) + 1e-06)
    ).astype(jnp.bfloat16)
    outgoing = normed[source].reshape(experts, cap, width)
    received = lax.all_to_all(outgoing, "fs", split_axis=0, concat_axis=0, tiled=True)
    senders, count, _ = received.shape
    rows = received.reshape(senders * count, width)
    first = jnp.dot(rows, gate_new[0], preferred_element_type=jnp.float32)
    second = jnp.dot(rows, up_new[0], preferred_element_type=jnp.float32)
    hidden = (jax.nn.silu(first) * second).astype(jnp.bfloat16)
    partial_out = jnp.dot(hidden, down_new[0], preferred_element_type=jnp.float32)
    summed = lax.psum_scatter(
        partial_out.reshape(senders, count, width).astype(jnp.bfloat16),
        "tp",
        scatter_dimension=2,
        tiled=True,
    )
    returned = lax.all_to_all(summed, "fs", split_axis=0, concat_axis=0, tiled=True)
    columns = returned.shape[2]
    route_out = returned.reshape(experts * cap, columns)[position].reshape(tok, 2, columns)
    mixed = jnp.sum(route_weights[:, :, None] * route_out.astype(jnp.float32), axis=1).astype(
        jnp.bfloat16
    )
    return (gate_new, up_new, down_new, mixed)


def place(n_z, n_y):
    f = lax.axis_index("fs")
    return lax.axis_index("gr"), f // n_y, lax.rem(f, n_y), lax.axis_index("tp")


def flip(z, k):
    return (z, z + 1 - 2 * lax.rem(z, 2), lax.rem(z + 2, 4), 3 - z)[k]


def device(c, z, y, x, n_y):
    return {"gr": c, "fs": z * n_y + y, "tp": x}


def greet(peers):
    barrier = pltpu.get_barrier_semaphore()
    for peer in peers:
        pl.semaphore_signal(barrier, inc=1, device_id=peer, device_id_type=MESH)
    pl.semaphore_wait(barrier, len(peers))


def remote(src, dst, send, recv, peer):
    return pltpu.make_async_remote_copy(
        src_ref=src, dst_ref=dst, send_sem=send, recv_sem=recv,
        device_id=peer, device_id_type=MESH,
    )


def sampler(
    n_z, n_y,
    tok_in, ids_in, rw_in, gain_in, gate_in, up_in, down_in,
    gate_out, up_out, down_out, mixed_out,
    wide, narrow, dwide, dnarrow, land, dland, dcross,
    normed, tok_s, rows, rw_s, rw_l, hid, out_s, ry_l, fin, ret,
    ld_sem, w_send, w_recv, f_send, f_recv,
    tz_send, tz_recv, ty_send, ty_recv, tx_send, tx_recv,
    rz_send, rz_recv, ry_send, ry_recv,
    h_send, h_recv, c_send, c_recv, y_send, y_recv, z_send, z_recv, o_sem,
):
    c, z, y, x = place(n_z, n_y)
    me = z * n_y + y
    n_fs = n_z * n_y
    g_rows, d_rows = gate_in.shape[1], down_in.shape[1]
    tok, width = tok_in.shape
    half = width // 2
    cap = tok // GROUPS
    hb = hid.shape[2]
    f32 = jnp.float32
    dev = functools.partial(device, n_y=n_y)
    ks = [(kz, 0) for kz in (1, 3, 2)] + [(kz, 1) for kz in (1, 3, 2, 0)] + [(0, 0)]
    last = len(ks) - 1
    at = []
    for kz, ky in ks:
        pz, py = flip(z, kz), (1 - y if ky else y)
        at.append((pz * n_y + py, dev(c, pz, py, x)))
    other = dev(1 - c, z, y, x)
    x_nbr = dev(c, z, y, 1 - x)
    y_nbr = dev(c, z, 1 - y, x)

    def xcols(i):
        return pl.ds(pl.multiple_of(i * half, half), half)

    def grow(core, f):
        return pl.ds(pl.multiple_of((core * n_fs + f) * g_rows, g_rows), g_rows)

    def drow(core, f):
        return pl.ds(pl.multiple_of((core * n_fs + f) * d_rows, d_rows), d_rows)

    def trow(f):
        return pl.ds(pl.multiple_of(f * cap, cap), cap)

    pair = (gate_in, up_in)
    loads = {}
    for n, (p, _) in enumerate(at):
        for i in range(2):
            loads[n, i] = pltpu.make_async_copy(pair[i].at[p], wide.at[i, n], ld_sem.at[3 * n + i])
            loads[n, i].start()
    for n, (p, _) in enumerate(at):
        loads[n, 2] = pltpu.make_async_copy(down_in.at[p], dwide.at[n], ld_sem.at[3 * n + 2])
        loads[n, 2].start()
    greet([d for _, d in at[:last]] + [other, x_nbr])

    def column(row, count):
        lanes = row.shape[1]
        eye = (lax.broadcasted_iota(jnp.int32, (count, lanes), 0)
               == lax.broadcasted_iota(jnp.int32, (count, lanes), 1))
        return jnp.sum(jnp.where(eye, row, 0.0), axis=1, keepdims=True)

    gain = column(gain_in[...], g_rows)
    arrive = {}
    onward = {}

    def fold(n):
        p, peer = at[n]
        for i in range(2):
            loads[n, i].wait()
            value = (wide[i, n] * gain).astype(BF16)
            if n == last:
                land[i, grow(c, me)] = value
                block = land.at[i, grow(c, me)]
                onward[n, i] = remote(block, block, f_send.at[3 * n + i], f_recv.at[3 * n + i], other)
                onward[n, i].start()
            else:
                narrow[i, n] = value
                cp = remote(narrow.at[i, n], land.at[i, grow(c, me)],
                            w_send.at[3 * n + i], w_recv.at[3 * n + i], peer)
                cp.start()
                arrive[n, i] = cp

    for n in range(HEAD):
        fold(n)

    def norm_rows(i, carry):
        r = pl.ds(pl.multiple_of(i * cap, cap), cap)
        v = tok_in[r, :].astype(f32)
        scale = lax.rsqrt(jnp.mean(v * v, axis=-1, keepdims=True) + 1e-06)
        normed[r, :] = (tok_in[r, xcols(x)].astype(f32) * scale).astype(BF16)
        return carry

    lax.fori_loop(0, GROUPS, norm_rows, 0)
    epg = gate_in.shape[0] // GROUPS
    low = ids_in[0:1, :]
    group = jnp.zeros_like(low)
    for g in range(1, GROUPS):
        group += (low >= g * epg).astype(jnp.int32)
    ahead = low == group * epg
    w_a, w_b = rw_in[0:1, :], rw_in[1:2, :]
    sub = lax.broadcasted_iota(jnp.int32, (8, tok), 0)
    w_of = jnp.where(sub == 0, jnp.where(ahead, w_a, w_b),
                     jnp.where(sub == 1, jnp.where(ahead, w_b, w_a), 0.0))
    onehot = (lax.broadcasted_iota(jnp.int32, (8, tok), 0) == group).astype(f32)
    upto = (lax.broadcasted_iota(jnp.int32, (tok, tok), 0)
            <= lax.broadcasted_iota(jnp.int32, (tok, tok), 1)).astype(BF16)
    count = jnp.dot(onehot.astype(BF16), upto, preferred_element_type=f32)
    slot = jnp.sum(onehot * count, axis=0, keepdims=True).astype(jnp.int32) - 1
    position = group * cap + slot

    def picked(g):
        return lax.broadcasted_iota(jnp.int32, (cap, tok), 0) + g * cap == position

    tz, rz, ty, tx, ry = {}, {}, {}, {}, {}
    for kz in (1, 3, 2, 0):
        g = flip(z, kz)
        pick = picked(g)
        block = jnp.dot(pick.astype(BF16), normed[...], preferred_element_type=f32).astype(BF16)
        w_row = lax.dot_general(w_of, pick.astype(f32), (((1,), (1,)), ((), ())),
                                precision=lax.Precision.HIGHEST, preferred_element_type=f32)
        if kz:
            tok_s[kz] = block
            rw_s[kz, :, :cap] = w_row
            peer = dev(c, g, y, x)
            tz[kz] = remote(tok_s.at[kz], rows.at[trow(me), xcols(x)],
                            tz_send.at[kz], tz_recv.at[kz], peer)
            tz[kz].start()
            rz[kz] = remote(rw_s.at[kz], rw_l.at[me], rz_send.at[kz], rz_recv.at[kz], peer)
            rz[kz].start()
        else:
            rows[trow(me), xcols(x)] = block
            rw_l[me, :, :cap] = w_row

    def pass_on(kz):
        src = flip(z, kz) * n_y + y
        block = rows.at[trow(src), xcols(x)]
        ty[kz] = remote(block, block, ty_send.at[kz], ty_recv.at[kz], y_nbr)
        ty[kz].start()
        tx[kz] = remote(block, block, tx_send.at[kz], tx_recv.at[kz], x_nbr)
        tx[kz].start()
        ry[kz] = remote(rw_l.at[src], rw_l.at[src], ry_send.at[kz], ry_recv.at[kz], y_nbr)
        ry[kz].start()

    pass_on(0)
    for n in list(range(HEAD, MID)) + [last]:
        fold(n)
    for kz in (1, 3, 2):
        tz[kz].wait_recv()
        rz[kz].wait_recv()
        pass_on(kz)
    for n in range(MID, last):
        fold(n)
    for n, (p, peer) in enumerate(at):
        loads[n, 2].wait()
        value = dwide[n].astype(BF16)
        if n == last:
            dland[drow(c, me)] = value
            block = dland.at[drow(c, me)]
            onward[n, 2] = remote(block, block, f_send.at[3 * n + 2], f_recv.at[3 * n + 2], other)
            onward[n, 2].start()
        else:
            dnarrow[n] = value
            arrive[n, 2] = remote(dnarrow.at[n], dland.at[drow(c, me)],
                                  w_send.at[3 * n + 2], w_recv.at[3 * n + 2], peer)
            arrive[n, 2].start()

    for kz in (0, 1, 3, 2):
        ty[kz].wait_recv()
        block = rows.at[trow(flip(z, kz) * n_y + 1 - y), xcols(x)]
        tx[4 + kz] = remote(block, block, tx_send.at[4 + kz], tx_recv.at[4 + kz], x_nbr)
        tx[4 + kz].start()

    order = sorted(range(last), key=lambda n: ks[n])
    for n in order:
        for i in range(2):
            arrive[n, i].wait_recv()
            block = land.at[i, grow(c, at[n][0])]
            onward[n, i] = remote(block, block, f_send.at[3 * n + i], f_recv.at[3 * n + i], other)
            onward[n, i].start()
    for cp in list(tx.values()) + list(ry.values()):
        cp.wait_recv()
    for n in [last] + order:
        for i in range(2):
            onward[n, i].wait_recv()
    outs = []
    for i, out in enumerate((gate_out, up_out)):
        cp = pltpu.make_async_copy(land.at[i], out.at[0], o_sem.at[i])
        cp.start()
        outs.append(cp)

    m = n_y * cap
    q = min(hb, 256)
    hsend = []
    for n, kz in enumerate(RETURN):
        r = pl.ds(pl.multiple_of(flip(z, kz) * m, m), m)

        def units(i, carry):
            s = pl.ds(pl.multiple_of(i * q, q), q)
            a = jnp.dot(rows[r, :], land[0, :, s], preferred_element_type=f32)
            b = jnp.dot(rows[r, :], land[1, :, s], preferred_element_type=f32)
            hid[x, r, s] = (a / (1.0 + jnp.exp(-a)) * b).astype(BF16)
            return carry

        lax.fori_loop(0, hb // q, units, 0)
        cp = remote(hid.at[x, r], hid.at[x, r], h_send.at[n], h_recv.at[n], x_nbr)
        cp.start()
        hsend.append(cp)

    for n in order:
        arrive[n, 2].wait_recv()
        block = dland.at[drow(c, at[n][0])]
        onward[n, 2] = remote(block, block, f_send.at[3 * n + 2], f_recv.at[3 * n + 2], other)
        onward[n, 2].start()
    for n in [last] + order:
        onward[n, 2].wait_recv()
    part = hb // 2
    mine = pl.ds(pl.multiple_of(c * part, part), part)
    cross = remote(
        dland.at[pl.ds(pl.multiple_of((1 - x) * hb + c * part, part), part)],
        dcross.at[mine], c_send.at[0], c_recv.at[0], x_nbr)
    cross.start()
    cp = pltpu.make_async_copy(
        dland.at[pl.ds(pl.multiple_of(x * hb, hb), hb)], down_out.at[0, :, xcols(x)], o_sem.at[2])
    cp.start()
    outs.append(cp)

    piece = half // PIECES
    ysend = {}
    zsend = []

    def give_back(n):
        kz = RETURN[n]
        for h in range(PIECES):
            d = pl.ds(h * piece, piece)
            ysend[n, h].wait_recv()
            total = (out_s[n, 1, :, d].astype(f32) + ry_l[n, :, d].astype(f32)).astype(BF16)
            if kz:
                i = n * PIECES + h
                fin[n, :, d] = total
                cp = remote(fin.at[n, :, d], ret.at[trow(z), d], z_send.at[i], z_recv.at[i],
                            dev(c, flip(z, kz), y, x))
                cp.start()
                zsend.append(cp)
            else:
                ret[trow(z), d] = total

    for n, kz in enumerate(RETURN):
        zs = flip(z, kz)
        hsend[n].wait_recv()
        for step in range(2):
            s = 1 - y if step == 0 else y
            f = zs * n_y + s
            w = jnp.where(y == 0, rw_l[f, 0:1, :], rw_l[f, 1:2, :])
            lane = lax.broadcasted_iota(jnp.int32, w.shape, 1)
            w = column(jnp.where(lane < cap, w, 0.0), cap)
            for h in range(PIECES):
                d = pl.ds(h * piece, piece)
                acc = jnp.dot(hid[0, trow(f)], dland[:hb, d], preferred_element_type=f32)
                acc += jnp.dot(hid[1, trow(f)], dland[hb:, d], preferred_element_type=f32)
                out_s[n, step, :, d] = (acc * w).astype(BF16)
                if step == 0:
                    i = n * PIECES + h
                    cp = remote(out_s.at[n, 0, :, d], ry_l.at[n, :, d],
                                y_send.at[i], y_recv.at[i], y_nbr)
                    cp.start()
                    ysend[n, h] = cp
        if n:
            give_back(n - 1)
    give_back(len(RETURN) - 1)

    cross.wait_recv()
    over = remote(dcross.at[mine], dcross.at[mine], c_send.at[1], c_recv.at[1], other)
    over.start()
    for cp in zsend:
        cp.wait_recv()
    everyone = (lax.broadcasted_iota(jnp.int32, (tok, tok), 0) == position).astype(BF16)
    mixed_out[...] = lax.dot_general(
        everyone, ret[...], (((0,), (0,)), ((), ())), preferred_element_type=f32).astype(BF16)
    over.wait_recv()
    cp = pltpu.make_async_copy(dcross, down_out.at[0, :, xcols(1 - x)], o_sem.at[3])
    cp.start()
    outs.append(cp)
    for cp in outs:
        cp.wait()
    for group_of in (arrive, onward, tz, rz, ty, tx, ry):
        for cp in group_of.values():
            cp.wait_send()
    for cp in hsend + list(ysend.values()) + zsend + [cross, over]:
        cp.wait_send()


def paired(n_z, n_y, tokens, route_ids, route_weights, norm_gain, gate_weight, up_weight, down_weight):
    tok, width = tokens.shape
    cap = tok // GROUPS
    half = width // lax.axis_size("tp")
    n_fs = n_z * n_y
    d_rows, d_cols = down_weight.shape[1:]
    g_rows, g_cols = gate_weight.shape[1:]
    f32 = jnp.float32

    hbm = pl.BlockSpec(memory_space=pl.ANY)
    vmem = pl.BlockSpec(memory_space=pltpu.VMEM)
    dma = pltpu.SemaphoreType.DMA
    lanes = -(-cap // 128) * 128
    gate_new, up_new, down_new, mixed = pl.pallas_call(
        functools.partial(sampler, n_z, n_y),
        out_shape=(
            jax.ShapeDtypeStruct((1, 2 * n_fs * g_rows, g_cols), BF16),
            jax.ShapeDtypeStruct((1, 2 * n_fs * g_rows, g_cols), BF16),
            jax.ShapeDtypeStruct((1, n_fs * d_rows, 2 * d_cols), BF16),
            jax.ShapeDtypeStruct((tok, half), BF16),
        ),
        in_specs=[vmem] * 4 + [pl.BlockSpec(memory_space=pltpu.HBM)] * 3,
        out_specs=(hbm, hbm, hbm, vmem),
        scratch_shapes=[
            pltpu.VMEM((2, n_fs, g_rows, g_cols), f32),
            pltpu.VMEM((2, n_fs - 1, g_rows, g_cols), BF16),
            pltpu.VMEM((n_fs, d_rows, d_cols), f32),
            pltpu.VMEM((n_fs - 1, d_rows, d_cols), BF16),
            pltpu.VMEM((2, 2 * n_fs * g_rows, g_cols), BF16),
            pltpu.VMEM((2 * n_fs * d_rows, d_cols), BF16),
            pltpu.VMEM((n_fs * d_rows, d_cols), BF16),
            pltpu.VMEM((tok, half), BF16),
            pltpu.VMEM((4, cap, half), BF16),
            pltpu.VMEM((n_fs * cap, width), BF16),
            pltpu.VMEM((4, 8, lanes), f32),
            pltpu.VMEM((n_fs, 8, lanes), f32),
            pltpu.VMEM((2, n_fs * cap, n_fs * d_rows), BF16),
            pltpu.VMEM((4, 2, cap, half), BF16),
            pltpu.VMEM((4, cap, half), BF16),
            pltpu.VMEM((4, cap, half), BF16),
            pltpu.VMEM((GROUPS * cap, half), BF16),
            dma((3 * n_fs,)),
            dma((3 * n_fs,)), dma((3 * n_fs,)), dma((3 * n_fs,)), dma((3 * n_fs,)),
            dma((4,)), dma((4,)), dma((4,)), dma((4,)), dma((8,)), dma((8,)),
            dma((4,)), dma((4,)), dma((4,)), dma((4,)),
            dma((4,)), dma((4,)), dma((2,)), dma((2,)), dma((4 * PIECES,)), dma((4 * PIECES,)),
            dma((4 * PIECES,)), dma((4 * PIECES,)), dma((4,)),
        ],
        compiler_params=pltpu.CompilerParams(
            collective_id=0, has_side_effects=True, vmem_limit_bytes=44 * 1024 * 1024),
    )(tokens, route_ids.T, route_weights.T, norm_gain.reshape(1, g_rows), gate_weight, up_weight, down_weight)
    return gate_new, up_new, down_new, mixed


def solution(mesh):
    placed = (
        P(("gr", "fs"), None),
        P(("gr", "fs"), None),
        P(("gr", "fs"), None),
        P(("gr", "fs")),
        P(None, ("gr", "fs"), "tp"),
        P(None, ("gr", "fs"), "tp"),
        P(None, ("gr", "fs"), "tp"),
    )
    n_fs = mesh.shape["fs"]

    def body(*args):
        experts = args[4].shape[0]
        if experts == n_fs == 2 * GROUPS and mesh.shape["gr"] == mesh.shape["tp"] == 2:
            return paired(GROUPS, 2, *args)
        return local(*args)

    return jax.shard_map(
        body,
        mesh=mesh,
        in_specs=placed,
        out_specs=(
            P("fs", None, "tp"),
            P("fs", None, "tp"),
            P("fs", "tp", None),
            P(("gr", "fs"), "tp"),
        ),
        check_vma=False,
    )
```
